32 devices in a mesh: gr: 2 (over x), fs: 4 (over z), tp: 4 (over y, core).
Axes of the slice: x: 2, y: 2, z: 4, core: 2. Of those that a mesh axis runs over, the one named last changes fastest.
Arguments:
- tokens: bfloat16 [1536, 4096], P(('gr', 'fs'), 'tp'), may hold values from -6 to 6
- route_ids: int32 [1536, 2], P(('gr', 'fs')), may hold values from 0 to 3, all different within a row; in each aligned block of 192 rows (0 to 191, 192 to 383, ...) at most 192 rows name the same one
- route_logits: float32 [1536, 2], P(('gr', 'fs')), may hold values from -6 to 6
- gain: float32 [4096], P(('gr', 'fs')), may hold values from 0.1 to 1.9
- gate_master: float32 [4, 4096, 2048], P(None, ('gr', 'fs'), 'tp'), may hold values from -6 to 6
- up_master: float32 [4, 4096, 2048], P(None, ('gr', 'fs'), 'tp'), may hold values from -6 to 6
- down_master: float32 [4, 2048, 4096], P(None, ('gr', 'fs'), 'tp'), may hold values from -6 to 6
Outputs:
- gate_weight: bfloat16 [4, 4096, 2048], P('fs', None, 'tp')
- up_weight: bfloat16 [4, 4096, 2048], P('fs', None, 'tp')
- down_weight: bfloat16 [4, 2048, 4096], P('fs', 'tp')
- mixed_out: bfloat16 [1536, 4096], P(('gr', 'fs'), 'tp')
The draws below stay inside these ranges and needn't reach their ends.
Inputs may be any that keep to these rules, and one draw needn't show every extreme that they name: `route_ids`: each row names 2 different experts; among the rows of one device no expert is named by more than 192 rows, a bound that some block reaches.
All inputs are finite; a program needn't handle non-finite values.
Results may differ from the reference program's by a relative error of at most 0.015.
Values may be sent and summed in bfloat16 or wider, within the bound.
A program may use at most 128 MiB of HBM per device.

```python
import math
import jax
import jax.numpy as jnp
import numpy as np
from jax import lax

D = 4096
FF = 2048
TOP = 2
TOK_DEV = 192
EXPERTS = 4
CAP = 192
TOKENS = 1536
N_GR = 2
N_FS = 4
N_TP = 4


def levels(rng, extent, pieces, low, largest):
    def one(position, shards_of):
        draws = jax.random.uniform(jax.random.fold_in(jax.random.fold_in(rng, 6), position), (shards_of,), jnp.float32, low / len(pieces), largest / len(pieces))
        return jnp.repeat(jnp.exp(draws), extent[position] // shards_of).reshape((-1,) + (1,) * (len(extent) - position - 1))

    level = one(*pieces[0])
    for cut in pieces[1:]:
        level = level * one(*cut)
    return level


def deal_out(key, own, number, rows, number_of, top, most, skew):
    order = jax.random.permutation(key, number_of)
    packed, ordinary = portions_of(number_of, rows * top, most, skew, True), portions_of(number_of, rows * top, most, skew, False)
    places = jnp.arange(number_of)

    def named(tallies, offset_by):
        used = int((tallies > 0).sum())
        fixed = max(1, used // 4)
        passed = fixed + (places - fixed + offset_by * (used - fixed)) % max(1, number_of - fixed)
        return jnp.zeros((number_of,), jnp.int32).at[order[jnp.where(places < fixed, places, passed)]].set(jnp.asarray(tallies, jnp.int32))

    tallies = jnp.where(number % 4 == 0, named(packed, number // 4), named(ordinary, number - number // 4 - 1))
    mixed = jax.random.permutation(jax.random.fold_in(own, 3), number_of)
    source_of, taker = mixed[0:number_of // 2 * 2:2], mixed[1:number_of // 2 * 2:2]
    margin = jnp.minimum(tallies[source_of] - 1, most - tallies[taker]) // 2
    margin = jnp.where((source_of == order[0]) | (taker == order[0]) | (tallies[taker] == 0), 0, jnp.maximum(margin, 0))
    passed = jax.random.randint(jax.random.fold_in(own, 4), (number_of // 2,), 0, 1 << 20) % (margin + 1)
    tallies = tallies.at[source_of].add(-passed).at[taker].add(passed)
    items = jnp.searchsorted(jnp.cumsum(tallies), jnp.arange(rows * top), side="right").astype(jnp.int32)
    table = items.reshape(top, rows).T
    table = table[jax.random.permutation(jax.random.fold_in(own, 1), rows)]
    offset_by = jax.random.randint(jax.random.fold_in(own, 2), (rows, 1), 0, top)
    return jnp.take_along_axis(table, (jnp.arange(top)[None, :] + offset_by) % top, axis=1)


def portions_of(amount, total, bound, skew, full):
    weights = [(1 << 20) // math.isqrt(standing ** skew) + 1 for standing in range(1, amount + 1)]
    largest = bound if full else min(bound, max(-(-total // amount), total * weights[0] // sum(weights)))
    least = 1 if total - largest >= amount - 1 else 0
    given, spare = [largest] + [least] * (amount - 1), total - largest - least * (amount - 1)
    while spare > 0:
        candidates = [i for i in range(1, amount) if given[i] < largest] or [i for i in range(1, amount) if given[i] < bound]
        mass, remaining = sum([weights[i] for i in candidates]), spare
        for i in candidates:
            more = min(bound - given[i], max(1, remaining * weights[i] // mass), spare)
            given[i] = given[i] + more
            spare = spare - more
    return np.array(given)


def bell_draw(key, extent, spread, reach, shards=(), held_as=jnp.bfloat16):
    values = jax.random.normal(key, extent, jnp.float32) * spread
    if len(shards) > 0:
        values = levels(key, extent, shards, -0.22, 0.18) * values
    return jnp.clip(values, min=-reach, max=reach).astype(held_as)


def setup_inputs(seed: int = 0) -> dict:
    seeds = jax.random.split(jax.random.key(seed), 8)
    tokens = bell_draw(seeds[0], (TOKENS, D), 1.0, 6.0, ((0, 8), (1, 4)))
    route_ids_keys = jax.random.split(jax.random.fold_in(seeds[1], 1), TOKENS // TOK_DEV)
    route_ids_turns = jax.random.permutation(jax.random.fold_in(seeds[1], 3), TOKENS // TOK_DEV)
    route_ids = jax.vmap(lambda own, number: deal_out(jax.random.fold_in(seeds[1], 2), own, number, TOK_DEV, EXPERTS, TOP, CAP, 2))(route_ids_keys, route_ids_turns).reshape((TOKENS, TOP))
    route_logits = bell_draw(seeds[2], (TOKENS, TOP), 1.5, 6.0, ((0, 8),), jnp.float32)
    gain = jnp.clip(1.0 + 0.18 * jax.random.normal(seeds[3], (D,), jnp.float32), 0.1, 1.9)
    gate_master = bell_draw(seeds[4], (EXPERTS, D, FF), 1.0, 6.0, ((1, 8), (2, 4)), jnp.float32)
    up_master = bell_draw(seeds[5], (EXPERTS, D, FF), 1.0, 6.0, ((1, 8), (2, 4)), jnp.float32)
    down_master = bell_draw(seeds[6], (EXPERTS, FF, D), 1.0, 6.0, ((1, 8), (2, 4)), jnp.float32)
    return dict(tokens=tokens, route_ids=route_ids, route_logits=route_logits, gain=gain, gate_master=gate_master, up_master=up_master, down_master=down_master)


EPS = 1e-06

def reference(tokens, route_ids, route_logits, gain, gate_master, up_master, down_master):
    row_gain = gain[None, :, None]
    gate_weight = (gate_master * row_gain).astype(jnp.bfloat16)
    up_weight = (up_master * row_gain).astype(jnp.bfloat16)
    down_weight = down_master.astype(jnp.bfloat16)
    float_rows = tokens.astype(jnp.float32)
    normed = (float_rows * lax.rsqrt(lax.optimization_barrier(jnp.mean(float_rows * float_rows, axis=1, keepdims=True)) + EPS)).astype(jnp.bfloat16)
    sigmoid_vals = jax.nn.sigmoid(route_logits.astype(jnp.float32))
    shares = sigmoid_vals / lax.optimization_barrier(jnp.sum(sigmoid_vals, axis=1, keepdims=True))
    assign_count = TOKENS * TOP
    slot_limit = N_GR * N_FS * CAP
    flattened = route_ids.reshape(assign_count).astype(jnp.int32)
    sort_order = jnp.argsort(flattened).astype(jnp.int32)
    starts = jnp.searchsorted(flattened[sort_order], jnp.arange(EXPERTS, dtype=jnp.int32), side='left').astype(jnp.int32)
    padded_order = jnp.concatenate([sort_order, jnp.full((slot_limit,), assign_count, jnp.int32)])
    padded_ids = jnp.concatenate([flattened, jnp.full((1,), -1, jnp.int32)])
    padded_shares = jnp.concatenate([shares.reshape(assign_count), jnp.zeros((1,), jnp.float32)])
    padded_rows = jnp.concatenate([normed, jnp.zeros((1, D), jnp.bfloat16)], axis=0)

    def one_expert(expert):
        picked_index = lax.dynamic_slice_in_dim(padded_order, starts[expert], slot_limit)
        is_valid = padded_ids[picked_index] == expert
        token_index = jnp.where(is_valid, picked_index // TOP, TOKENS).astype(jnp.int32)
        expert_rows = padded_rows[token_index]
        gate_value = jnp.dot(expert_rows, gate_weight[expert], preferred_element_type=jnp.float32) * D ** (-0.5)
        up_value = jnp.dot(expert_rows, up_weight[expert], preferred_element_type=jnp.float32) * D ** (-0.5)
        hidden = (jax.nn.silu(gate_value) * up_value).astype(jnp.bfloat16)
        hidden_blocks = hidden.reshape(slot_limit, N_TP, FF // N_TP).astype(jnp.float32)
        down_blocks = down_weight[expert].reshape(N_TP, FF // N_TP, D).astype(jnp.float32)
        partials = jnp.einsum('mjf,jfd->jmd', hidden_blocks, down_blocks).astype(jnp.bfloat16)
        partials = lax.optimization_barrier(partials)
        expert_out = (lax.optimization_barrier(jnp.sum(partials.astype(jnp.float32), axis=0)) * FF ** (-0.5)).astype(jnp.bfloat16)
        expert_out = lax.optimization_barrier(expert_out)
        weights_here = jnp.where(is_valid, padded_shares[picked_index], jnp.float32(0.0))
        return (token_index, expert_out.astype(jnp.float32) * weights_here[:, None])
    token_lists, terms = lax.map(one_expert, jnp.arange(EXPERTS, dtype=jnp.int32))
    total = jnp.zeros((TOKENS + 1, D), jnp.float32).at[token_lists.reshape(-1)].add(terms.reshape(-1, D))
    mixed_out = total[:TOKENS].astype(jnp.bfloat16)
    return (gate_weight, up_weight, down_weight, mixed_out)
```

```python
import functools

import jax
import jax.numpy as jnp
from jax import lax
from jax.experimental import pallas as pl
from jax.experimental.pallas import tpu as pltpu
from jax.sharding import PartitionSpec as P

EPS = 1e-06
MESH = pl.DeviceIdType.MESH


def greet(sizes):
    barrier = pltpu.get_barrier_semaphore()
    count = 0
    for name, size in sizes:
        me = lax.axis_index(name)
        for off in range(1, size):
            other = lax.rem(me + off, size)
            pl.semaphore_signal(barrier, inc=1, device_id={name: other}, device_id_type=MESH)
            count += 1
    pl.semaphore_wait(barrier, count)


def step_order(n_fs):
    return sorted(range(1, n_fs), key=lambda s: (-min(s, n_fs - s), s))


def spread(n_gr, n_fs, src, dst, zs, zr, xs, xr, ls):
    g, f = lax.axis_index("gr"), lax.axis_index("fs")
    own = dst.shape[0]
    rows = src.shape[1]

    def place(gg, s):
        return dst.at[:, pl.ds(pl.multiple_of((gg * n_fs + s) * rows, rows), rows), :]

    def piece(e):
        return src.at[pl.ds(e * own, own)]

    sends = {}
    for step in step_order(n_fs):
        p = lax.rem(f + step, n_fs)
        copy = pltpu.make_async_remote_copy(
            src_ref=piece(p),
            dst_ref=place(g, f),
            send_sem=zs.at[step],
            recv_sem=zr.at[step],
            device_id={"fs": p},
            device_id_type=MESH,
        )
        copy.start()
        sends[step] = copy
    local = pltpu.make_async_copy(piece(f), place(g, f), ls)
    local.start()

    forwards = {}

    def forward(step):
        s = lax.rem(f + n_fs - step, n_fs)
        for o in range(1, n_gr):
            copy = pltpu.make_async_remote_copy(
                src_ref=piece(f) if step == 0 else place(g, s),
                dst_ref=place(g, s),
                send_sem=xs.at[o - 1, step],
                recv_sem=xr.at[o - 1, step],
                device_id={"gr": lax.rem(g + o, n_gr)},
                device_id_type=MESH,
            )
            copy.start()
            forwards[o, step] = copy

    forward(0)
    return sends, local, forward, forwards


def pair_kernel(n_gr, n_fs, a, b, a_out, b_out, zs, zr, xs, xr, ls):
    greet((("gr", n_gr), ("fs", n_fs)))
    states = [
        spread(n_gr, n_fs, src, dst, zs.at[m], zr.at[m], xs.at[m], xr.at[m], ls.at[m])
        for m, (src, dst) in enumerate(((a, a_out), (b, b_out)))
    ]
    for sends, _, forward, _ in states:
        for step in step_order(n_fs):
            sends[step].wait_recv()
            forward(step)
    for sends, local, _, forwards in states:
        local.wait()
        for copy in sends.values():
            copy.wait_send()
        for copy in forwards.values():
            copy.wait_send()
            copy.wait_recv()


def down_kernel(n_gr, n_fs, n_tp, a, cols_out, rows_out, held, zs, zr, xs, xr, ls, ys, yr, ks):
    greet((("gr", n_gr), ("fs", n_fs), ("tp", n_tp)))
    g, f, t = lax.axis_index("gr"), lax.axis_index("fs"), lax.axis_index("tp")
    rows, width = a.shape[1], a.shape[2]
    per = n_gr * n_fs // n_tp
    sends, local, forward, forwards = spread(n_gr, n_fs, a, held, zs, zr, xs, xr, ls)
    handed = []

    def hand(o, step):
        b = lax.rem(g + n_gr - o, n_gr) * n_fs + lax.rem(f + n_fs - step, n_fs)
        j, i = b // per, lax.rem(b, per)
        src = held.at[:, pl.ds(pl.multiple_of(b * rows, rows), rows), :]
        dst = rows_out.at[
            :,
            pl.ds(pl.multiple_of(i * rows, rows), rows),
            pl.ds(pl.multiple_of(t * width, width), width),
        ]
        stay = pltpu.make_async_copy(src, dst, ks.at[o, step])
        go = pltpu.make_async_remote_copy(
            src_ref=src,
            dst_ref=dst,
            send_sem=ys.at[o, step],
            recv_sem=yr.at[lax.rem(j + n_tp - t, n_tp), i],
            device_id={"tp": j},
            device_id_type=MESH,
        )

        @pl.when(j == t)
        def _():
            stay.start()

        @pl.when(j != t)
        def _():
            go.start()

        handed.append((j, stay, go))

    local.wait()
    hand(0, 0)
    for step in step_order(n_fs):
        sends[step].wait_recv()
        forward(step)
        hand(0, step)
    for (o, step), copy in forwards.items():
        copy.wait_recv()
        hand(o, step)
    whole = pltpu.make_async_copy(held, cols_out, ls)
    whole.start()
    for copy in sends.values():
        copy.wait_send()
    for copy in forwards.values():
        copy.wait_send()
    for j, stay, go in handed:

        @pl.when(j == t)
        def _():
            stay.wait()

        @pl.when(j != t)
        def _():
            go.wait_send()

    for k in range(1, n_tp):
        source = lax.rem(t + n_tp - k, n_tp)
        for i in range(per):
            pltpu.make_async_remote_copy(
                src_ref=held.at[:, pl.ds(i * rows, rows), :],
                dst_ref=rows_out.at[
                    :, pl.ds(i * rows, rows), pl.ds(pl.multiple_of(source * width, width), width)
                ],
                send_sem=ys.at[0, 0],
                recv_sem=yr.at[k, i],
                device_id={"tp": source},
                device_id_type=MESH,
            ).wait_recv()
    whole.wait()


def exchange_pair(a, b, n_gr, n_fs):
    experts, rows, width = a.shape
    out = jax.ShapeDtypeStruct((experts // n_fs, n_gr * n_fs * rows, width), a.dtype)
    dma = pltpu.SemaphoreType.DMA
    size = a.size * 2
    return pl.pallas_call(
        functools.partial(pair_kernel, n_gr, n_fs),
        out_shape=(out, out),
        in_specs=[pl.BlockSpec(memory_space=pltpu.VMEM)] * 2,
        out_specs=(pl.BlockSpec(memory_space=pl.ANY),) * 2,
        scratch_shapes=[
            dma((2, n_fs)),
            dma((2, n_fs)),
            dma((2, n_gr - 1, n_fs)),
            dma((2, n_gr - 1, n_fs)),
            dma((2,)),
        ],
        compiler_params=pltpu.CompilerParams(collective_id=1, has_side_effects=True),
        cost_estimate=pl.CostEstimate(flops=0, bytes_accessed=size * 80, transcendentals=0),
        name="pair_exchange",
    )(a, b)


def exchange_down(a, n_gr, n_fs, n_tp):
    experts, rows, width = a.shape
    own = experts // n_fs
    full = n_gr * n_fs * rows
    dma = pltpu.SemaphoreType.DMA
    size = a.size * 2
    return pl.pallas_call(
        functools.partial(down_kernel, n_gr, n_fs, n_tp),
        out_shape=(
            jax.ShapeDtypeStruct((own, full, width), a.dtype),
            jax.ShapeDtypeStruct((own, full // n_tp, width * n_tp), a.dtype),
        ),
        in_specs=[pl.BlockSpec(memory_space=pltpu.VMEM)],
        out_specs=(pl.BlockSpec(memory_space=pl.ANY),) * 2,
        scratch_shapes=[
            pltpu.VMEM((own, full, width), a.dtype),
            dma((n_fs,)),
            dma((n_fs,)),
            dma((n_gr - 1, n_fs)),
            dma((n_gr - 1, n_fs)),
            dma(()),
            dma((n_gr, n_fs)),
            dma((n_tp, n_gr * n_fs // n_tp)),
            dma((n_gr, n_fs)),
        ],
        compiler_params=pltpu.CompilerParams(collective_id=2, has_side_effects=True),
        cost_estimate=pl.CostEstimate(flops=0, bytes_accessed=size * 40, transcendentals=0),
        name="down_exchange",
    )(a)


def body(n_gr, n_fs, n_tp, tokens, route_ids, route_logits, gain, gate_master, up_master, down_master):
    experts = gate_master.shape[0]
    own = experts // n_fs
    model_width = gate_master.shape[1] * n_gr * n_fs
    hidden_width = gate_master.shape[2] * n_tp
    row_gain = gain[None, :, None]
    gate_cast = (gate_master * row_gain).astype(jnp.bfloat16)
    up_cast = (up_master * row_gain).astype(jnp.bfloat16)
    down_cast = down_master.astype(jnp.bfloat16)

    float_rows = tokens.astype(jnp.float32)
    squares = lax.psum(jnp.sum(float_rows * float_rows, axis=1, keepdims=True), "tp")
    normed = (float_rows * lax.rsqrt(squares / model_width + EPS)).astype(jnp.bfloat16)
    group = lax.all_gather(normed, "fs", axis=0, tiled=True)
    blocks = lax.all_gather(group, "tp", axis=0)

    sigmoid_vals = jax.nn.sigmoid(route_logits)
    shares = sigmoid_vals / jnp.sum(sigmoid_vals, axis=1, keepdims=True)
    chosen = route_ids[:, :, None] == jnp.arange(experts, dtype=jnp.int32)[None, None, :]
    weights = jnp.sum(jnp.where(chosen, shares[:, :, None], 0.0), axis=1)
    all_weights = lax.all_gather(weights, "fs", axis=0, tiled=True)

    gate_full, up_full = exchange_pair(gate_cast, up_cast, n_gr, n_fs)
    width = tokens.shape[1]
    scale_in = model_width ** (-0.5)

    def project(matrix):
        return sum(
            jnp.dot(
                blocks[j],
                matrix[j * width : (j + 1) * width],
                preferred_element_type=jnp.float32,
            )
            for j in range(n_tp)
        )

    hidden = []
    for e in range(own):
        gate_value = project(gate_full[e]) * scale_in
        up_value = project(up_full[e]) * scale_in
        hidden.append((jax.nn.silu(gate_value) * up_value).astype(jnp.bfloat16))
    hidden = jnp.stack(hidden)
    down_cast, hidden = lax.optimization_barrier((down_cast, hidden))
    all_hidden = lax.all_gather(hidden, "tp", axis=0)
    down_cols, down_rows = exchange_down(down_cast, n_gr, n_fs, n_tp)

    part = hidden.shape[2]
    first = lax.axis_index("fs") * own
    total = 0.0
    for e in range(own):
        summed = sum(
            jnp.dot(
                all_hidden[j, e],
                down_cols[e, j * part : (j + 1) * part],
                preferred_element_type=jnp.float32,
            )
            for j in range(n_tp)
        )
        share = lax.dynamic_slice_in_dim(all_weights, first + e, 1, axis=1)
        total = total + summed * hidden_width ** (-0.5) * share
    mixed_out = lax.psum_scatter(
        total.astype(jnp.bfloat16), "fs", scatter_dimension=0, tiled=True
    )
    return (gate_full, up_full, down_rows, mixed_out)


def solution(mesh):
    in_specs = (
        P(("gr", "fs"), "tp"),
        P(("gr", "fs"), None),
        P(("gr", "fs"), None),
        P(("gr", "fs")),
        P(None, ("gr", "fs"), "tp"),
        P(None, ("gr", "fs"), "tp"),
        P(None, ("gr", "fs"), "tp"),
    )
    out_specs = (
        P("fs", None, "tp"),
        P("fs", None, "tp"),
        P("fs", "tp", None),
        P(("gr", "fs"), "tp"),
    )
    sizes = (mesh.shape["gr"], mesh.shape["fs"], mesh.shape["tp"])
    return jax.shard_map(
        functools.partial(body, *sizes), mesh=mesh, in_specs=in_specs, out_specs=out_specs, check_vma=False
    )
```
